32 devices in a mesh: grp: 2 (over y), sp: 4 (over z), tp: 4 (over x, core).
Axes of the slice: x: 2, y: 2, z: 4, core: 2. Of those that a mesh axis runs over, the one named last changes fastest.
Arguments:
- tokens: bfloat16 [2048, 2048], P(('grp', 'sp'), 'tp'), parts along dimension 0, may hold values from -40 to 40
- norm_gain: float32 [2, 2048], replicated, may hold values from 0.1 to 1.9
- value_proj: bfloat16 [2, 1024, 2048], P(None, 'tp', 'sp'), may hold values from -0.125 to 0.125
- gate_proj: bfloat16 [2, 1024, 2048], P(None, 'tp', 'sp'), may hold values from -0.125 to 0.125
- conv_taps: float32 [2, 4, 1024], P(None, None, 'tp'), may hold values from -3 to 3
- recur_map: bfloat16 [2, 16, 64, 64], P(None, 'tp'), may hold values from -0.75 to 0.75
- input_map: bfloat16 [2, 16, 64, 64], P(None, 'tp'), may hold values from -0.75 to 0.75
- decay_param: float32 [2, 1024], P(None, 'tp'), may hold values from 3 to 16
- decay_offset: float32 [2, 1024, 1024], P(None, 'tp', 'sp'), may hold values from -3 to 0
- mix_proj: bfloat16 [2, 1024, 2048], P(None, 'sp', 'tp'), may hold values from -0.1875 to 0.1875
Outputs:
- mixed_out: bfloat16 [2048, 2048], P(('grp', 'sp'), 'tp'), parts along dimension 0
The draws below stay inside these ranges and needn't reach their ends.
There are 2 independent parts, one for each index of `grp`. The reference program is written for one: setup_inputs(seed, part) draws one part's arguments, and reference() takes and returns one part's arrays. A program takes and returns all parts, laid end to end along the dimension named above; an argument that names none is the same for every part. Nothing has to cross between parts.
All inputs are finite; a program needn't handle non-finite values.
Results may differ from the reference program's by a relative error of at most 0.013.
Values may be sent and summed in bfloat16 or wider, within the bound.
A program may use at most 64 MiB of HBM per device.

```python
import jax
import jax.numpy as jnp
from jax import lax

D = 2048
HEADS = 16
D_LRU = 1024
HEAD_DIM = 64
CONV = 4
LAYERS = 2
TOK_DEV = 256
LENGTH = 1024


def channel_rates(key):
    base = jax.random.fold_in(key, 11)
    keys = jax.random.split(base, 3)
    shape = (LAYERS, D // 2)
    share = 0.5
    fastest = jax.random.uniform(keys[0], shape, jnp.float32) < share
    short_span = min(30, TOK_DEV // 4) * 1.0
    long_span = min(100, TOK_DEV // 2) * 1.0
    fast_span = jnp.exp(jax.random.uniform(keys[1], shape, jnp.float32, jnp.log(short_span), jnp.log(long_span)))
    slow_rate = jnp.exp(jax.random.uniform(keys[2], shape, jnp.float32, jnp.log(0.01), jnp.log(0.04))) / LENGTH
    return jnp.where(fastest, 0.25 / fast_span, slow_rate)


def draw_decay_param(key, part):
    rates = channel_rates(key)
    return -jnp.log(jnp.expm1(rates))


def draw_decay_offset(key, part):
    rates = channel_rates(key)
    keys = jax.random.split(jax.random.fold_in(key, 23), 3)
    blocks = LENGTH // TOK_DEV
    stretch = jnp.exp(jax.random.uniform(keys[0], (LAYERS, D // 2, blocks), jnp.float32, 0.0, jnp.log(3.0)))
    stretch = jnp.repeat(stretch, TOK_DEV, axis=2)
    reference_level = -4.0 * rates[:, :, None] * (stretch - 1.0)
    slot_positions = jax.random.randint(keys[1], (LAYERS, 3), 0, LENGTH)
    share_part = jax.random.uniform(keys[2], (LAYERS, 3, D // 2), jnp.float32, 0.2, 0.5)
    match_count = (slot_positions[:, :, None] == jnp.arange(LENGTH)[None, None, :]).astype(jnp.float32)
    spike_groups = jnp.einsum('rkv,rkq->rvq', jnp.log1p(-share_part), match_count)
    return (reference_level + spike_groups).astype(jnp.float32)


def draw_tokens(key, part):
    keys = jax.random.split(key, 3)
    noise = jnp.clip(jax.random.normal(keys[0], (LENGTH, D), jnp.float32), -4.0, 4.0)
    row_scale = jnp.exp(jax.random.uniform(keys[1], (LENGTH, 1), jnp.float32, 0.0, jnp.log(10.0))) / 5.0
    column_upper = 3.0
    position = jnp.arange(D, dtype=jnp.float32)[None, :] / D
    jitter = jax.random.uniform(keys[2], (1, D), jnp.float32, -0.3, 0.3)
    column_scale = jnp.exp(jnp.log(column_upper) * position + jitter)
    return (noise * row_scale * column_scale).astype(jnp.bfloat16)


def steps_of(own_key, dims, cuts, low, top_value):
    gain = 1.0
    for dim, blocks in cuts:
        steps = jax.random.uniform(jax.random.fold_in(jax.random.fold_in(own_key, 6), dim), (blocks,), jnp.float32, low / len(cuts), top_value / len(cuts))
        gain = gain * jnp.repeat(jnp.exp(steps), dims[dim] // blocks).reshape((-1,) + (1,) * (len(dims) - 1 - dim))
    return gain


def gaussian(stream_key, dims, spread, most, shards=(), held_as=jnp.bfloat16):
    level = steps_of(stream_key, dims, shards, -0.22, 0.18) if shards else 1.0
    result = jax.random.normal(stream_key, dims, jnp.float32) * spread * level
    return jnp.minimum(jnp.maximum(result, -most), most).astype(held_as)


def setup_inputs(seed: int = 0, part: int = 0) -> dict:
    streams_of = jax.random.split(jax.random.key(seed), 11)
    own_keys = jax.random.split(jax.random.fold_in(streams_of[10], part), 11)
    return {
        "tokens": draw_tokens(jax.random.fold_in(jax.random.fold_in(streams_of[10], part), 71), part),
        "norm_gain": jnp.clip(1.0 + 0.18 * jax.random.normal(streams_of[1], (LAYERS, D), jnp.float32), 0.1, 1.9),
        "value_proj": gaussian(streams_of[2], (LAYERS, D_LRU, D), D ** -0.5, 0.125, ((1, 4), (2, 4))),
        "gate_proj": gaussian(streams_of[3], (LAYERS, D_LRU, D), D ** -0.5, 0.125, ((1, 4), (2, 4))),
        "conv_taps": gaussian(streams_of[4], (LAYERS, CONV, D_LRU), CONV ** -0.5, 3.0, ((2, 4),), jnp.float32),
        "recur_map": gaussian(streams_of[5], (LAYERS, HEADS, HEAD_DIM, HEAD_DIM), HEAD_DIM ** -0.5, 0.75, ((1, 4),)),
        "input_map": gaussian(streams_of[6], (LAYERS, HEADS, HEAD_DIM, HEAD_DIM), HEAD_DIM ** -0.5, 0.75, ((1, 4),)),
        "decay_param": draw_decay_param(jax.random.fold_in(streams_of[10], 71), part),
        "decay_offset": draw_decay_offset(jax.random.fold_in(streams_of[10], 71), part),
        "mix_proj": gaussian(streams_of[9], (LAYERS, D_LRU, D), D_LRU ** -0.5, 0.1875, ((1, 4), (2, 4))),
    }


EPS = 1e-06
RATE_SCALE = 8.0

def combine_pairs(earlier, later):
    return (earlier[0] * later[0], later[0] * earlier[1] + later[1])

def mixer_layer(residual, gain_row, value_weights, gate_weights, taps_layer, recur_layer, input_layer, param_layer, offset_layer, mix_weights):
    wide = residual.astype(jnp.float32)
    scale_factor = lax.rsqrt(lax.optimization_barrier(jnp.mean(wide * wide, axis=1)) + EPS)
    scaled = (wide * gain_row[None, :]).astype(jnp.bfloat16)
    value_rows = (jnp.dot(value_weights, scaled.T, preferred_element_type=jnp.float32) * scale_factor[None, :]).astype(jnp.bfloat16)
    gate_rows = (jnp.dot(gate_weights, scaled.T, preferred_element_type=jnp.float32) * scale_factor[None, :]).astype(jnp.bfloat16)
    padded = jnp.concatenate([jnp.zeros((D_LRU, CONV - 1), jnp.bfloat16), value_rows], axis=1)
    smoothed = jnp.zeros((D_LRU, LENGTH), jnp.float32)
    for tap_index in range(CONV):
        smoothed = smoothed + taps_layer[tap_index][:, None] * padded[:, tap_index:tap_index + LENGTH].astype(jnp.float32)
    smoothed_half = smoothed.astype(jnp.bfloat16).astype(jnp.float32).reshape(HEADS, HEAD_DIM, LENGTH)
    recur = jax.nn.sigmoid(jnp.einsum('hit,hij->hjt', smoothed_half, recur_layer.astype(jnp.float32)).reshape(D_LRU, LENGTH))
    inputs = jax.nn.sigmoid(jnp.einsum('hit,hij->hjt', smoothed_half, input_layer.astype(jnp.float32)).reshape(D_LRU, LENGTH))
    log_decay = -RATE_SCALE * recur * jax.nn.softplus(-param_layer)[:, None] + offset_layer
    decay = jnp.exp(log_decay)
    driving = jnp.sqrt(-jnp.expm1(2.0 * log_decay)) * inputs * smoothed
    _, hidden_state = lax.associative_scan(combine_pairs, (decay, driving), axis=1)
    branch = (hidden_state * jax.nn.silu(gate_rows.astype(jnp.float32))).astype(jnp.bfloat16)
    projected = jnp.dot(branch.T, mix_weights, preferred_element_type=jnp.float32)
    return (wide + projected).astype(jnp.bfloat16)

def reference(tokens, norm_gain, value_proj, gate_proj, conv_taps, recur_map, input_map, decay_param, decay_offset, mix_proj):
    residual = tokens
    for layer_index in range(LAYERS):
        residual = mixer_layer(residual, norm_gain[layer_index], value_proj[layer_index], gate_proj[layer_index], conv_taps[layer_index], recur_map[layer_index], input_map[layer_index], decay_param[layer_index], decay_offset[layer_index], mix_proj[layer_index])
    return residual
```

```python
import functools
import math

import jax
import jax.numpy as jnp
from jax import lax
from jax.experimental import pallas as pl
from jax.experimental.pallas import tpu as pltpu
from jax.sharding import PartitionSpec as P

EPS = 1e-06
RATE_SCALE = 8.0
HALO = 16
MESH = pl.DeviceIdType.MESH
NT = (((1,), (1,)), ((), ()))


def softplus(v):
    u = jnp.exp(-jnp.abs(v))
    series = jnp.full_like(u, 1.0 / 9.0)
    for term in range(8, 0, -1):
        series = 1.0 / term - u * series
    return jnp.maximum(v, 0.0) + jnp.where(u < 0.1, u * series, jnp.log(1.0 + u))


def one_minus_exp(y, exp_y):
    series = jnp.full_like(y, 1.0)
    for term in range(8, 1, -1):
        series = 1.0 + y * series * (1.0 / term)
    return jnp.where(y > -0.5, -y * series, 1.0 - exp_y)


def sigmoid(v):
    return 1.0 / (1.0 + jnp.exp(-v))


def kernel(
    groups, sp_count, tp_count, layers,
    tokens, gains, value, gate, taps_ref, recur, inmap, param, offset, mix, out,
    vbuf, gbuf, mbuf, scbuf, ssbuf, brbuf, halo_out, halo_in, end_out, end_in, carry, blocks, offs, wide,
    zsend, zrecv, ysend, yrecv, gsend, grecv, fsend, ssend, srecv, sfsend, bsend, brecv, bfsend,
    hsend, hrecv, csend, crecv,
):
    grp, me, tp = lax.axis_index("grp"), lax.axis_index("sp"), lax.axis_index("tp")
    rows, own_cols = tokens.shape
    channels = value.shape[1]
    head = recur.shape[2]
    heads = recur.shape[1]
    tap_total = taps_ref.shape[1]
    paired = tp_count % 2 == 0
    partner = tp + 1 - 2 * lax.rem(tp, 2)

    same = [lax.rem(tp + 2 * k, tp_count) for k in range(1, tp_count // 2)] if paired else [
        lax.rem(tp + k, tp_count) for k in range(1, tp_count)]
    same_from = [lax.rem(tp + tp_count - 2 * k, tp_count) for k in range(1, tp_count // 2)] if paired else [
        lax.rem(tp + tp_count - k, tp_count) for k in range(1, tp_count)]
    other_groups = [lax.rem(grp + k, groups) for k in range(1, groups)]
    group_from = [lax.rem(grp + groups - k, groups) for k in range(1, groups)]

    barrier = pltpu.get_barrier_semaphore()
    greeted = 0
    for peer in same + ([partner] if paired else []):
        pl.semaphore_signal(barrier, inc=1, device_id={"tp": peer}, device_id_type=MESH)
        greeted += 1
    for k in range(1, sp_count):
        pl.semaphore_signal(barrier, inc=1, device_id={"sp": lax.rem(me + k, sp_count)}, device_id_type=MESH)
        greeted += 1
    for peer in other_groups:
        pl.semaphore_signal(barrier, inc=1, device_id={"grp": peer}, device_id_type=MESH)
        greeted += 1
    pl.semaphore_wait(barrier, greeted)

    def remote(src, dst, send, recv, axis, peer):
        return pltpu.make_async_remote_copy(
            src_ref=src, dst_ref=dst, send_sem=send, recv_sem=recv, device_id={axis: peer}, device_id_type=MESH)

    class Gather:
        def __init__(self, buf, layer, cuts, sems):
            self.buf, self.layer, self.sems = buf, layer, sems
            size = buf.shape[2] // cuts
            self.views = [pl.ds(c * size, size) for c in range(cuts)]

        def copy(self, cut, slot, sem, number, peer):
            part = self.buf.at[self.layer, slot, self.views[cut]]
            return remote(part, part, sem.at[self.layer, cut, number], self.sems[1].at[self.layer, cut, slot], "tp", peer)

        def start(self):
            for cut in range(len(self.views)):
                for number, peer in enumerate(same):
                    self.copy(cut, tp, self.sems[0], number, peer).start()
                if paired:
                    self.copy(cut, tp, self.sems[0], len(same), partner).start()

        def finish(self):
            for cut in range(len(self.views)):
                for number, source in enumerate(same_from):
                    self.copy(cut, source, self.sems[0], number, partner).wait_recv()
                    if paired:
                        self.copy(cut, source, self.sems[2], number, partner).start()
            if paired:
                for cut in range(len(self.views)):
                    self.copy(cut, partner, self.sems[0], 0, partner).wait_recv()
                    for number in range(len(same)):
                        source = lax.rem(partner + tp_count - 2 * (number + 1), tp_count)
                        self.copy(cut, source, self.sems[0], number, partner).wait_recv()

        def drain(self):
            for cut in range(len(self.views)):
                for number in range(len(same) + (1 if paired else 0)):
                    self.copy(cut, tp, self.sems[0], number, partner).wait_send()
                if paired:
                    for number, source in enumerate(same_from):
                        self.copy(cut, source, self.sems[2], number, partner).wait_send()

    parts = []
    for layer in range(layers):
        parts += [(value, vbuf, layer), (gate, gbuf, layer), (mix, mbuf, layer)]

    def share(number):
        size = parts[number][0].shape[1] // groups
        return pl.ds(pl.multiple_of(grp * size, size), size)

    def z_copy(number, way, step):
        own, buf, layer = parts[number]
        source = me - way * (step - 1)
        src = own.at[layer, share(number)] if step == 1 else buf.at[layer, source, share(number)]
        valid = (source >= 0) & (source < sp_count) & (me + way >= 0) & (me + way < sp_count)
        slot = jnp.clip(source, 0, sp_count - 1)
        if step > 1:
            src = buf.at[layer, slot, share(number)]
        copy = remote(src, buf.at[layer, slot, share(number)], zsend.at[number, (way + 1) // 2, step - 1],
                      zrecv.at[number, slot], "sp", jnp.clip(me + way, 0, sp_count - 1))
        return valid, copy

    def y_copy(number, source, which, peer):
        _, buf, layer = parts[number]
        part = buf.at[layer, source, share(number)]
        return remote(part, part, ysend.at[number, source, which], yrecv.at[number, source, which], "grp", peer)

    def own_send(number):
        for way in (1, -1):
            valid, copy = z_copy(number, way, 1)
            pl.when(valid)(copy.start)

    def pump(number, third):
        per = -(-(sp_count - 1) // 3)
        for step in range(third * per + 1, min((third + 1) * per, sp_count - 1) + 1):
            for way in (1, -1):
                source = me - way * step
                valid = (source >= 0) & (source < sp_count)
                slot = jnp.clip(source, 0, sp_count - 1)
                _, buf, layer = parts[number]

                @pl.when(valid)
                def _():
                    part = buf.at[layer, slot, share(number)]
                    remote(part, part, zsend.at[number, 0, 0], zrecv.at[number, slot], "sp",
                           lax.rem(me + 1, sp_count)).wait_recv()
                    for which, peer in enumerate(other_groups):
                        y_copy(number, slot, which, peer).start()

                if step < sp_count - 1:
                    going, copy = z_copy(number, way, step + 1)
                    pl.when(going)(copy.start)

    def y_wait(number):
        _, buf, layer = parts[number]
        size = parts[number][0].shape[1] // groups
        for k in range(1, sp_count):
            source = lax.rem(me + k, sp_count)
            for which, peer in enumerate(group_from):
                part = buf.at[layer, source, pl.ds(pl.multiple_of(peer * size, size), size)]
                remote(part, part, ysend.at[number, source, which], yrecv.at[number, source, which],
                       "grp", other_groups[0]).wait_recv()

    gathers = []

    def normed(layer):
        x = wide[...]
        own_gain = gains[layer, :, pl.ds(pl.multiple_of(tp * own_cols, own_cols), own_cols)]
        scbuf[layer, tp] = (x * own_gain).astype(jnp.bfloat16)
        ssbuf[layer, tp] = lax.dot_general(
            jnp.ones((8, own_cols), jnp.float32), x * x, NT,
            precision=lax.Precision.HIGHEST, preferred_element_type=jnp.float32)
        small = Gather(ssbuf, layer, 1, (ssend, srecv, sfsend))
        large = Gather(scbuf, layer, 2, (gsend, grecv, fsend))
        gathers.extend([small, large])
        small.start()
        large.start()
        return small, large

    def project(layer, buf):
        cols = buf.shape[3]
        chunk = math.gcd(cols, own_cols)
        total = None
        for at in range(0, cols * sp_count, chunk):
            left = scbuf[layer, at // own_cols, :, at % own_cols : at % own_cols + chunk]
            right = buf[layer, at // cols, :, at % cols : at % cols + chunk]
            term = lax.dot_general(left, right, NT, preferred_element_type=jnp.float32)
            total = term if total is None else total + term
        return total

    wide[...] = tokens[...].astype(jnp.float32)
    pending = normed(0)
    for number in range(3):
        own_send(number)
    for layer in range(layers):
        vbuf[layer, me] = value[layer]
        gbuf[layer, me] = gate[layer]
        mbuf[layer, me] = mix[layer]
        offs[layer] = offset[layer].T
        for kind, source in enumerate((recur, inmap)):
            blocks[layer, kind] = jnp.zeros((channels, channels), jnp.bfloat16)
            for number in range(heads):
                cut = slice(number * head, (number + 1) * head)
                blocks[layer, kind, cut, cut] = source[layer, number]

    for layer in range(layers):
        first = 3 * layer
        more = layer + 1 < layers
        if layer == 0:
            for number in (first, first + 1):
                pump(number, 0)
            if more:
                own_send(first + 3)
                own_send(first + 4)
            for number in (first, first + 1):
                pump(number, 1)
            pump(first + 2, 0)
        for gather in pending:
            gather.finish()
        for number in (first, first + 1):
            pump(number, 2)
        if layer > 0:
            pump(first + 2, 0)
        y_wait(first)
        y_wait(first + 1)
        squares = ssbuf[layer, 0]
        for source in range(1, tp_count):
            squares = squares + ssbuf[layer, source]
        scale = lax.rsqrt(squares / (own_cols * tp_count) + EPS).T[:, 0:1]
        value_half = (project(layer, vbuf) * scale).astype(jnp.bfloat16)
        halo_out[layer] = value_half[rows - HALO :]
        halo_copy = remote(halo_out.at[layer], halo_in.at[layer], hsend.at[layer], hrecv.at[layer], "sp",
                           jnp.minimum(me + 1, sp_count - 1))
        pl.when(me < sp_count - 1)(halo_copy.start)
        gate_rows = (project(layer, gbuf) * scale).astype(jnp.bfloat16).astype(jnp.float32)
        silu = gate_rows / (1.0 + jnp.exp(-gate_rows))
        pump(first + 2, 1)
        if more:
            own_send(first + 5)

        @pl.when(me == 0)
        def _():
            halo_in[layer] = jnp.zeros((HALO, channels), jnp.bfloat16)

        pl.when(me > 0)(halo_copy.wait_recv)
        longer = jnp.concatenate(
            [halo_in[layer].astype(jnp.float32), value_half.astype(jnp.float32)], axis=0)
        smoothed = jnp.zeros((rows, channels), jnp.float32)
        for tap in range(tap_total):
            behind = tap_total - 1 - tap
            shifted = pltpu.roll(longer, behind, 0) if behind else longer
            smoothed = smoothed + taps_ref[layer, tap : tap + 1, :] * shifted[HALO:]
        half = smoothed.astype(jnp.bfloat16)
        recur_gate = sigmoid(jnp.dot(half, blocks[layer, 0], preferred_element_type=jnp.float32))
        input_gate = sigmoid(jnp.dot(half, blocks[layer, 1], preferred_element_type=jnp.float32))
        rate = -RATE_SCALE * softplus(-param[layer])
        log_decay = recur_gate * rate + offs[layer]
        a = jnp.exp(log_decay)
        b = jnp.sqrt(one_minus_exp(2.0 * log_decay, a * a)) * input_gate * smoothed
        index = lax.broadcasted_iota(jnp.int32, (rows, channels), 0)
        reach = 1
        while reach < rows:
            inside = index >= reach
            b = b + a * jnp.where(inside, pltpu.roll(b, reach, 0), 0.0)
            a = a * jnp.where(inside, pltpu.roll(a, reach, 0), 1.0)
            reach *= 2
        end_out[layer, 0:8] = a[rows - 8 :]
        end_out[layer, 8:16] = b[rows - 8 :]
        for k in range(1, sp_count):
            peer = jnp.minimum(me + k, sp_count - 1)
            pl.when(me + k < sp_count)(
                remote(end_out.at[layer], end_in.at[layer, me], csend.at[layer, k - 1], crecv.at[layer, me],
                       "sp", peer).start)
        pump(first + 2, 2)
        if more:
            pump(first + 3, 0)
            pump(first + 4, 0)
        carry[...] = jnp.zeros((8, channels), jnp.float32)
        for source in range(sp_count - 1):

            @pl.when(source < me)
            def _():
                remote(end_out.at[layer], end_in.at[layer, source], csend.at[layer, 0], crecv.at[layer, source],
                       "sp", lax.rem(me + 1, sp_count)).wait_recv()
                carry[...] = end_in[layer, source, 0:8] * carry[...] + end_in[layer, source, 8:16]
                carry[...] = jnp.broadcast_to(carry[7:8], (8, channels))

        brbuf[layer, tp] = ((b + a * carry[0:1]) * silu).astype(jnp.bfloat16)
        branches = Gather(brbuf, layer, 1, (bsend, brecv, bfsend))
        gathers.append(branches)
        branches.start()
        if more:
            pump(first + 3, 1)
            pump(first + 4, 1)
        y_wait(first + 2)
        branches.finish()
        chunk_rows = mbuf.shape[2]
        chunk = math.gcd(chunk_rows, channels)
        total = wide[...]
        for at in range(0, channels * tp_count, chunk):
            total = total + jnp.dot(
                brbuf[layer, at // channels, :, at % channels : at % channels + chunk],
                mbuf[layer, at // chunk_rows, at % chunk_rows : at % chunk_rows + chunk, :],
                preferred_element_type=jnp.float32)
        rounded = total.astype(jnp.bfloat16)
        if more:
            wide[...] = rounded.astype(jnp.float32)
            pending = normed(layer + 1)
        else:
            out[...] = rounded

    for gather in gathers:
        gather.drain()
    for number in range(len(parts)):
        for step in range(1, sp_count):
            for way in (1, -1):
                valid, copy = z_copy(number, way, step)
                pl.when(valid)(copy.wait_send)
            source = lax.rem(me + step, sp_count)
            for which, peer in enumerate(other_groups):
                y_copy(number, source, which, peer).wait_send()
    for layer in range(layers):
        pl.when(me < sp_count - 1)(
            remote(halo_out.at[layer], halo_in.at[layer], hsend.at[layer], hrecv.at[layer], "sp",
                   jnp.minimum(me + 1, sp_count - 1)).wait_send)
        for k in range(1, sp_count):
            pl.when(me + k < sp_count)(
                remote(end_out.at[layer], end_in.at[layer, me], csend.at[layer, k - 1], crecv.at[layer, me],
                       "sp", jnp.minimum(me + k, sp_count - 1)).wait_send)


def local(sizes, tokens, norm_gain, value_proj, gate_proj, conv_taps, recur_map, input_map, decay_param,
          decay_offset, mix_proj):
    groups, sp_count, tp_count = sizes
    layers = value_proj.shape[0]
    rows, own_cols = tokens.shape
    channels = value_proj.shape[1]
    bf, f32 = jnp.bfloat16, jnp.float32
    same = tp_count // 2
    dma = pltpu.SemaphoreType.DMA
    count = 3 * layers
    peers = max(groups - 1, 1)
    direct, fwd = tp_count, max(same, 1)
    scratch = [
        pltpu.VMEM((layers, sp_count) + value_proj.shape[1:], bf),
        pltpu.VMEM((layers, sp_count) + gate_proj.shape[1:], bf),
        pltpu.VMEM((layers, sp_count) + mix_proj.shape[1:], bf),
        pltpu.VMEM((layers, tp_count, rows, own_cols), bf),
        pltpu.VMEM((layers, tp_count, 8, rows), f32),
        pltpu.VMEM((layers, tp_count, rows, channels), bf),
        pltpu.VMEM((layers, HALO, channels), bf),
        pltpu.VMEM((layers, HALO, channels), bf),
        pltpu.VMEM((layers, 16, channels), f32),
        pltpu.VMEM((layers, sp_count, 16, channels), f32),
        pltpu.VMEM((8, channels), f32),
        pltpu.VMEM((layers, 2, channels, channels), bf),
        pltpu.VMEM((layers, rows, channels), f32),
        pltpu.VMEM((rows, own_cols), f32),
        dma((count, 2, sp_count)), dma((count, sp_count)), dma((count, sp_count, peers)), dma((count, sp_count, peers)),
        dma((layers, 2, direct)), dma((layers, 2, tp_count)), dma((layers, 2, fwd)),
        dma((layers, 1, direct)), dma((layers, 1, tp_count)), dma((layers, 1, fwd)),
        dma((layers, 1, direct)), dma((layers, 1, tp_count)), dma((layers, 1, fwd)),
        dma((layers,)), dma((layers,)), dma((layers, sp_count)), dma((layers, sp_count)),
    ]
    vmem = pl.BlockSpec(memory_space=pltpu.VMEM)
    return pl.pallas_call(
        functools.partial(kernel, groups, sp_count, tp_count, layers),
        out_shape=jax.ShapeDtypeStruct((rows, own_cols), bf),
        in_specs=[vmem] * 10,
        out_specs=vmem,
        scratch_shapes=scratch,
        compiler_params=pltpu.CompilerParams(
            collective_id=0, has_side_effects=True, vmem_limit_bytes=60 * 1024 * 1024),
    )(tokens, norm_gain[:, None, :], value_proj, gate_proj, conv_taps, recur_map, input_map,
      decay_param[:, None, :], decay_offset, mix_proj)


def solution(mesh):
    in_specs = (
        P(("grp", "sp"), "tp"),
        P(),
        P(None, "tp", "sp"),
        P(None, "tp", "sp"),
        P(None, None, "tp"),
        P(None, "tp", None, None),
        P(None, "tp", None, None),
        P(None, "tp"),
        P(None, "tp", "sp"),
        P(None, "sp", "tp"),
    )
    out_specs = P(("grp", "sp"), "tp")
    sizes = (mesh.shape["grp"], mesh.shape["sp"], mesh.shape["tp"])
    return jax.shard_map(
        functools.partial(local, sizes), mesh=mesh, in_specs=in_specs, out_specs=out_specs, check_vma=False)
```

```python
import functools
import math

import jax
import jax.numpy as jnp
from jax import lax
from jax.experimental import pallas as pl
from jax.experimental.pallas import tpu as pltpu
from jax.sharding import PartitionSpec as P

EPS = 1e-06
RATE_SCALE = 8.0
HALO = 16
PIECES = 1
MESH = pl.DeviceIdType.MESH
NT = (((1,), (1,)), ((), ()))


def softplus(v):
    u = jnp.exp(-jnp.abs(v))
    series = jnp.full_like(u, 1.0 / 9.0)
    for term in range(8, 0, -1):
        series = 1.0 / term - u * series
    return jnp.maximum(v, 0.0) + jnp.where(u < 0.1, u * series, jnp.log(1.0 + u))


def one_minus_exp(y, exp_y):
    series = jnp.full_like(y, 1.0)
    for term in range(8, 1, -1):
        series = 1.0 + y * series * (1.0 / term)
    return jnp.where(y > -0.5, -y * series, 1.0 - exp_y)


def sigmoid(v):
    return 1.0 / (1.0 + jnp.exp(-v))


def kernel(
    groups, sp_count, tp_count, layers,
    tokens, gains, value, gate, taps_ref, recur, inmap, param, offset, mix, out,
    vbuf, gbuf, mbuf, scbuf, ssbuf, brbuf, halo_out, halo_in, end_out, end_in, carry, blocks, offs, wide,
    zsend, zrecv, ysend, yrecv, gsend, grecv, fsend, ssend, srecv, sfsend, bsend, brecv, bfsend,
    hsend, hrecv, csend, crecv,
):
    grp, me, tp = lax.axis_index("grp"), lax.axis_index("sp"), lax.axis_index("tp")
    rows, own_cols = tokens.shape
    channels = value.shape[1]
    head = recur.shape[2]
    heads = recur.shape[1]
    tap_total = taps_ref.shape[1]
    paired = tp_count % 2 == 0
    partner = tp + 1 - 2 * lax.rem(tp, 2)

    same = [lax.rem(tp + 2 * k, tp_count) for k in range(1, tp_count // 2)] if paired else [
        lax.rem(tp + k, tp_count) for k in range(1, tp_count)]
    same_from = [lax.rem(tp + tp_count - 2 * k, tp_count) for k in range(1, tp_count // 2)] if paired else [
        lax.rem(tp + tp_count - k, tp_count) for k in range(1, tp_count)]
    other_groups = [lax.rem(grp + k, groups) for k in range(1, groups)]
    group_from = [lax.rem(grp + groups - k, groups) for k in range(1, groups)]

    barrier = pltpu.get_barrier_semaphore()
    greeted = 0
    for peer in same + ([partner] if paired else []):
        pl.semaphore_signal(barrier, inc=1, device_id={"tp": peer}, device_id_type=MESH)
        greeted += 1
    for k in range(1, sp_count):
        pl.semaphore_signal(barrier, inc=1, device_id={"sp": lax.rem(me + k, sp_count)}, device_id_type=MESH)
        greeted += 1
    for peer in other_groups:
        pl.semaphore_signal(barrier, inc=1, device_id={"grp": peer}, device_id_type=MESH)
        greeted += 1
    pl.semaphore_wait(barrier, greeted)

    def remote(src, dst, send, recv, axis, peer):
        return pltpu.make_async_remote_copy(
            src_ref=src, dst_ref=dst, send_sem=send, recv_sem=recv, device_id={axis: peer}, device_id_type=MESH)

    class Gather:
        def __init__(self, buf, layer, cuts, sems):
            self.buf, self.layer, self.sems = buf, layer, sems
            size = buf.shape[2] // cuts
            self.views = [pl.ds(c * size, size) for c in range(cuts)]

        def copy(self, cut, slot, sem, number, peer):
            part = self.buf.at[self.layer, slot, self.views[cut]]
            return remote(part, part, sem.at[self.layer, cut, number], self.sems[1].at[self.layer, cut, slot], "tp", peer)

        def start(self):
            for cut in range(len(self.views)):
                for number, peer in enumerate(same):
                    self.copy(cut, tp, self.sems[0], number, peer).start()
                if paired:
                    self.copy(cut, tp, self.sems[0], len(same), partner).start()

        def finish(self):
            for cut in range(len(self.views)):
                for number, source in enumerate(same_from):
                    self.copy(cut, source, self.sems[0], number, partner).wait_recv()
                    if paired:
                        self.copy(cut, source, self.sems[2], number, partner).start()
            if paired:
                for cut in range(len(self.views)):
                    self.copy(cut, partner, self.sems[0], 0, partner).wait_recv()
                    for number in range(len(same)):
                        source = lax.rem(partner + tp_count - 2 * (number + 1), tp_count)
                        self.copy(cut, source, self.sems[0], number, partner).wait_recv()

        def drain(self):
            for cut in range(len(self.views)):
                for number in range(len(same) + (1 if paired else 0)):
                    self.copy(cut, tp, self.sems[0], number, partner).wait_send()
                if paired:
                    for number, source in enumerate(same_from):
                        self.copy(cut, source, self.sems[2], number, partner).wait_send()

    parts = []
    for layer in range(layers):
        for own, buf in ((value, vbuf), (gate, gbuf), (mix, mbuf)):
            parts += [(own, buf, layer)] * PIECES

    def share(number, carrier=grp):
        size = parts[number][0].shape[1] // (groups * PIECES)
        return pl.ds(pl.multiple_of((number % PIECES * groups + carrier) * size, size), size)

    def z_copy(number, way, step):
        own, buf, layer = parts[number]
        source = me - way * (step - 1)
        src = own.at[layer, share(number)] if step == 1 else buf.at[layer, source, share(number)]
        valid = (source >= 0) & (source < sp_count) & (me + way >= 0) & (me + way < sp_count)
        slot = jnp.clip(source, 0, sp_count - 1)
        if step > 1:
            src = buf.at[layer, slot, share(number)]
        copy = remote(src, buf.at[layer, slot, share(number)], zsend.at[number, (way + 1) // 2, step - 1],
                      zrecv.at[number, slot], "sp", jnp.clip(me + way, 0, sp_count - 1))
        return valid, copy

    def y_copy(number, source, which, peer):
        _, buf, layer = parts[number]
        part = buf.at[layer, source, share(number)]
        return remote(part, part, ysend.at[number, source, which], yrecv.at[number, source, which], "grp", peer)

    def own_send(base):
        for number in range(base * PIECES, (base + 1) * PIECES):
            for way in (1, -1):
                valid, copy = z_copy(number, way, 1)
                pl.when(valid)(copy.start)

    def pump(base, third):
        per = -(-(sp_count - 1) // 3)
        for step in range(third * per + 1, min((third + 1) * per, sp_count - 1) + 1):
            for number in range(base * PIECES, (base + 1) * PIECES):
                for way in (1, -1):
                    pump_piece(number, step, way)

    def pump_piece(number, step, way):
        source = me - way * step
        valid = (source >= 0) & (source < sp_count)
        slot = jnp.clip(source, 0, sp_count - 1)
        _, buf, layer = parts[number]

        @pl.when(valid)
        def _():
            part = buf.at[layer, slot, share(number)]
            remote(part, part, zsend.at[number, 0, 0], zrecv.at[number, slot], "sp",
                   lax.rem(me + 1, sp_count)).wait_recv()

        if step < sp_count - 1:
            going, copy = z_copy(number, way, step + 1)
            pl.when(going)(copy.start)

        @pl.when(valid)
        def _():
            for which, peer in enumerate(other_groups):
                y_copy(number, slot, which, peer).start()

    def y_wait(base):
        for number in range(base * PIECES, (base + 1) * PIECES):
            _, buf, layer = parts[number]
            for k in range(1, sp_count):
                source = lax.rem(me + k, sp_count)
                for which, peer in enumerate(group_from):
                    part = buf.at[layer, source, share(number, peer)]
                    remote(part, part, ysend.at[number, source, which], yrecv.at[number, source, which],
                           "grp", other_groups[0]).wait_recv()

    gathers = []

    def normed(layer):
        x = wide[...]
        own_gain = gains[layer, :, pl.ds(pl.multiple_of(tp * own_cols, own_cols), own_cols)]
        scbuf[layer, tp] = (x * own_gain).astype(jnp.bfloat16)
        ssbuf[layer, tp] = lax.dot_general(
            jnp.ones((8, own_cols), jnp.float32), x * x, NT,
            precision=lax.Precision.HIGHEST, preferred_element_type=jnp.float32)
        small = Gather(ssbuf, layer, 1, (ssend, srecv, sfsend))
        large = Gather(scbuf, layer, 2, (gsend, grecv, fsend))
        gathers.extend([small, large])
        small.start()
        large.start()
        return small, large

    def project(layer, buf):
        cols = buf.shape[3]
        chunk = math.gcd(cols, own_cols)
        total = None
        for at in range(0, cols * sp_count, chunk):
            left = scbuf[layer, at // own_cols, :, at % own_cols : at % own_cols + chunk]
            right = buf[layer, at // cols, :, at % cols : at % cols + chunk]
            term = lax.dot_general(left, right, NT, preferred_element_type=jnp.float32)
            total = term if total is None else total + term
        return total

    own_send(0)
    own_send(1)
    wide[...] = tokens[...].astype(jnp.float32)
    pending = normed(0)
    for layer in range(layers):
        vbuf[layer, me] = value[layer]
        gbuf[layer, me] = gate[layer]
        mbuf[layer, me] = mix[layer]
        offs[layer] = offset[layer].T
        for kind, source in enumerate((recur, inmap)):
            blocks[layer, kind] = jnp.zeros((channels, channels), jnp.bfloat16)
            for number in range(heads):
                cut = slice(number * head, (number + 1) * head)
                blocks[layer, kind, cut, cut] = source[layer, number]

    for layer in range(layers):
        first = 3 * layer
        more = layer + 1 < layers
        if layer == 0:
            pump(first, 0)
            pump(first + 1, 0)
            own_send(first + 2)
            for gather in pending:
                gather.finish()
            pump(first, 1)
            pump(first + 1, 1)
            if more:
                own_send(first + 3)
            pump(first + 2, 0)
            if more:
                own_send(first + 4)
            pump(first, 2)
            pump(first + 1, 2)
            pump(first + 2, 1)
        else:
            pump(first + 2, 0)
            pump(first, 2)
            for gather in pending:
                gather.finish()
            pump(first + 1, 2)
        y_wait(first)
        y_wait(first + 1)
        squares = ssbuf[layer, 0]
        for source in range(1, tp_count):
            squares = squares + ssbuf[layer, source]
        scale = lax.rsqrt(squares / (own_cols * tp_count) + EPS).T[:, 0:1]
        value_half = (project(layer, vbuf) * scale).astype(jnp.bfloat16)
        halo_out[layer] = value_half[rows - HALO :]
        halo_copy = remote(halo_out.at[layer], halo_in.at[layer], hsend.at[layer], hrecv.at[layer], "sp",
                           jnp.minimum(me + 1, sp_count - 1))
        pl.when(me < sp_count - 1)(halo_copy.start)
        gate_rows = (project(layer, gbuf) * scale).astype(jnp.bfloat16).astype(jnp.float32)
        silu = gate_rows / (1.0 + jnp.exp(-gate_rows))
        if more:
            own_send(first + 5)
            pump(first + 3, 0)
        if layer > 0:
            pump(first + 2, 1)

        @pl.when(me == 0)
        def _():
            halo_in[layer] = jnp.zeros((HALO, channels), jnp.bfloat16)

        pl.when(me > 0)(halo_copy.wait_recv)
        longer = jnp.concatenate(
            [halo_in[layer].astype(jnp.float32), value_half.astype(jnp.float32)], axis=0)
        smoothed = jnp.zeros((rows, channels), jnp.float32)
        for tap in range(tap_total):
            behind = tap_total - 1 - tap
            shifted = pltpu.roll(longer, behind, 0) if behind else longer
            smoothed = smoothed + taps_ref[layer, tap : tap + 1, :] * shifted[HALO:]
        half = smoothed.astype(jnp.bfloat16)
        recur_gate = sigmoid(jnp.dot(half, blocks[layer, 0], preferred_element_type=jnp.float32))
        input_gate = sigmoid(jnp.dot(half, blocks[layer, 1], preferred_element_type=jnp.float32))
        rate = -RATE_SCALE * softplus(-param[layer])
        log_decay = recur_gate * rate + offs[layer]
        a = jnp.exp(log_decay)
        b = jnp.sqrt(one_minus_exp(2.0 * log_decay, a * a)) * input_gate * smoothed
        index = lax.broadcasted_iota(jnp.int32, (rows, channels), 0)
        reach = 1
        while reach < rows:
            inside = index >= reach
            b = b + a * jnp.where(inside, pltpu.roll(b, reach, 0), 0.0)
            a = a * jnp.where(inside, pltpu.roll(a, reach, 0), 1.0)
            reach *= 2
        end_out[layer, 0:8] = a[rows - 8 :]
        end_out[layer, 8:16] = b[rows - 8 :]
        for k in range(1, sp_count):
            peer = jnp.minimum(me + k, sp_count - 1)
            pl.when(me + k < sp_count)(
                remote(end_out.at[layer], end_in.at[layer, me], csend.at[layer, k - 1], crecv.at[layer, me],
                       "sp", peer).start)
        pump(first + 2, 2)
        if more:
            pump(first + 4, 0)
        carry[...] = jnp.zeros((8, channels), jnp.float32)
        for source in range(sp_count - 1):

            @pl.when(source < me)
            def _():
                remote(end_out.at[layer], end_in.at[layer, source], csend.at[layer, 0], crecv.at[layer, source],
                       "sp", lax.rem(me + 1, sp_count)).wait_recv()
                carry[...] = end_in[layer, source, 0:8] * carry[...] + end_in[layer, source, 8:16]
                carry[...] = jnp.broadcast_to(carry[7:8], (8, channels))

        brbuf[layer, tp] = ((b + a * carry[0:1]) * silu).astype(jnp.bfloat16)
        branches = Gather(brbuf, layer, 1, (bsend, brecv, bfsend))
        gathers.append(branches)
        branches.start()
        if more:
            pump(first + 3, 1)
            pump(first + 4, 1)
        y_wait(first + 2)
        branches.finish()
        chunk_rows = mbuf.shape[2]
        chunk = math.gcd(chunk_rows, channels)
        total = wide[...]
        for at in range(0, channels * tp_count, chunk):
            total = total + jnp.dot(
                brbuf[layer, at // channels, :, at % channels : at % channels + chunk],
                mbuf[layer, at // chunk_rows, at % chunk_rows : at % chunk_rows + chunk, :],
                preferred_element_type=jnp.float32)
        rounded = total.astype(jnp.bfloat16)
        if more:
            wide[...] = rounded.astype(jnp.float32)
            pending = normed(layer + 1)
        else:
            out[...] = rounded

    for gather in gathers:
        gather.drain()
    for number in range(len(parts)):
        for step in range(1, sp_count):
            for way in (1, -1):
                valid, copy = z_copy(number, way, step)
                pl.when(valid)(copy.wait_send)
            source = lax.rem(me + step, sp_count)
            for which, peer in enumerate(other_groups):
                y_copy(number, source, which, peer).wait_send()
    for layer in range(layers):
        pl.when(me < sp_count - 1)(
            remote(halo_out.at[layer], halo_in.at[layer], hsend.at[layer], hrecv.at[layer], "sp",
                   jnp.minimum(me + 1, sp_count - 1)).wait_send)
        for k in range(1, sp_count):
            pl.when(me + k < sp_count)(
                remote(end_out.at[layer], end_in.at[layer, me], csend.at[layer, k - 1], crecv.at[layer, me],
                       "sp", jnp.minimum(me + k, sp_count - 1)).wait_send)


def local(sizes, tokens, norm_gain, value_proj, gate_proj, conv_taps, recur_map, input_map, decay_param,
          decay_offset, mix_proj):
    groups, sp_count, tp_count = sizes
    layers = value_proj.shape[0]
    rows, own_cols = tokens.shape
    channels = value_proj.shape[1]
    bf, f32 = jnp.bfloat16, jnp.float32
    same = tp_count // 2
    dma = pltpu.SemaphoreType.DMA
    count = 3 * layers * PIECES
    peers = max(groups - 1, 1)
    direct, fwd = tp_count, max(same, 1)
    scratch = [
        pltpu.VMEM((layers, sp_count) + value_proj.shape[1:], bf),
        pltpu.VMEM((layers, sp_count) + gate_proj.shape[1:], bf),
        pltpu.VMEM((layers, sp_count) + mix_proj.shape[1:], bf),
        pltpu.VMEM((layers, tp_count, rows, own_cols), bf),
        pltpu.VMEM((layers, tp_count, 8, rows), f32),
        pltpu.VMEM((layers, tp_count, rows, channels), bf),
        pltpu.VMEM((layers, HALO, channels), bf),
        pltpu.VMEM((layers, HALO, channels), bf),
        pltpu.VMEM((layers, 16, channels), f32),
        pltpu.VMEM((layers, sp_count, 16, channels), f32),
        pltpu.VMEM((8, channels), f32),
        pltpu.VMEM((layers, 2, channels, channels), bf),
        pltpu.VMEM((layers, rows, channels), f32),
        pltpu.VMEM((rows, own_cols), f32),
        dma((count, 2, sp_count)), dma((count, sp_count)), dma((count, sp_count, peers)), dma((count, sp_count, peers)),
        dma((layers, 2, direct)), dma((layers, 2, tp_count)), dma((layers, 2, fwd)),
        dma((layers, 1, direct)), dma((layers, 1, tp_count)), dma((layers, 1, fwd)),
        dma((layers, 1, direct)), dma((layers, 1, tp_count)), dma((layers, 1, fwd)),
        dma((layers,)), dma((layers,)), dma((layers, sp_count)), dma((layers, sp_count)),
    ]
    vmem = pl.BlockSpec(memory_space=pltpu.VMEM)
    return pl.pallas_call(
        functools.partial(kernel, groups, sp_count, tp_count, layers),
        out_shape=jax.ShapeDtypeStruct((rows, own_cols), bf),
        in_specs=[vmem] * 10,
        out_specs=vmem,
        scratch_shapes=scratch,
        compiler_params=pltpu.CompilerParams(
            collective_id=0, has_side_effects=True, vmem_limit_bytes=60 * 1024 * 1024),
    )(tokens, norm_gain[:, None, :], value_proj, gate_proj, conv_taps, recur_map, input_map,
      decay_param[:, None, :], decay_offset, mix_proj)


def solution(mesh):
    in_specs = (
        P(("grp", "sp"), "tp"),
        P(),
        P(None, "tp", "sp"),
        P(None, "tp", "sp"),
        P(None, None, "tp"),
        P(None, "tp", None, None),
        P(None, "tp", None, None),
        P(None, "tp"),
        P(None, "tp", "sp"),
        P(None, "sp", "tp"),
    )
    out_specs = P(("grp", "sp"), "tp")
    sizes = (mesh.shape["grp"], mesh.shape["sp"], mesh.shape["tp"])
    return jax.shard_map(
        functools.partial(local, sizes), mesh=mesh, in_specs=in_specs, out_specs=out_specs, check_vma=False)
```
